32 devices in a mesh: fs: 2 (over core), tp: 16 (over z, y, x).
Axes of the slice: x: 2, y: 2, z: 4, core: 2. Of those that a mesh axis runs over, the one named last changes fastest.
Arguments:
- trained_gate: float32 [16, 504, 2048], P(None, 'fs', 'tp'), may hold values from -0.125 to 0.125
- trained_up: float32 [16, 504, 2048], P(None, 'fs', 'tp'), may hold values from -0.125 to 0.125
- trained_down: float32 [16, 504, 2048], P(None, 'fs', 'tp'), may hold values from -0.25 to 0.25
- trained_shared_gate: float32 [504, 2048], P('fs', 'tp'), may hold values from -0.125 to 0.125
- trained_shared_up: float32 [504, 2048], P('fs', 'tp'), may hold values from -0.125 to 0.125
- trained_shared_down: float32 [504, 2048], P('fs', 'tp'), may hold values from -0.25 to 0.25
- ffn_gain: float32 [2048], P('tp'), may hold values from 0.1 to 1.9
- prompt_tokens: bfloat16 [512, 2048], P('fs'), may hold values from -6 to 6
- expert_ids: int32 [512, 8], P('fs'), may hold values from 0 to 15, all different within a row; in each aligned block of 256 rows (0 to 255, 256 to 511, ...) at most 256 rows name the same one
- route_scores: float32 [512, 8], P('fs'), may hold values from 0.05 to 1
Outputs:
- served_gate: bfloat16 [16, 504, 2048], P('tp')
- served_up: bfloat16 [16, 504, 2048], P('tp')
- served_down: bfloat16 [16, 504, 2048], P('tp')
- served_shared_gate: bfloat16 [504, 2048], P(None, 'tp')
- served_shared_up: bfloat16 [504, 2048], P(None, 'tp')
- served_shared_down: bfloat16 [504, 2048], P(None, 'tp')
- mixture_out: bfloat16 [512, 2048], P('fs', 'tp')
The draws below stay inside these ranges and needn't reach their ends.
Inputs may be any that keep to these rules, and one draw needn't show every extreme that they name: `expert_ids`: each row names 8 different experts, and every expert is named by some row. Within the 256 rows of one index of fs no expert is named by more than 256 rows, and in every draw some expert is named by exactly 256 rows of some index of fs.
All inputs are finite; a program needn't handle non-finite values.
Results may differ from the reference program's by a relative error of at most 0.0082.
Values may be sent and summed in bfloat16 or wider, within the bound.
No kernel may reach another device: no remote copies, remote signals or barrier semaphores. Data moves between devices by JAX's collectives and lax.ppermute only.
A program may use at most 64 MiB of HBM per device.

```python
import math
import jax
import jax.numpy as jnp
import numpy as np
from jax import lax

D = 2048
FF = 504
TOP_K = 8
TOK = 256
EXPERTS = 16
CAP = 256
TOKENS = 512
N_FS = 2


def level_of(key, shape, split, low, largest):
    gain = 1.0
    for axis_at, parts in split:
        heights = jax.random.uniform(jax.random.fold_in(jax.random.fold_in(key, 6), axis_at), (parts,), jnp.float32, low / len(split), largest / len(split))
        gain = gain * jnp.repeat(jnp.exp(heights), shape[axis_at] // parts).reshape((-1,) + (1,) * (len(shape) - 1 - axis_at))
    return gain


def assign_block(key, own, number, rows, count, top, reach, lean):
    order = jax.random.permutation(key, count)
    crowded, common = shares(count, rows * top, reach, lean, True), shares(count, rows * top, reach, lean, False)
    places = jnp.arange(count)

    def named(lengths, rotation):
        used = int((lengths > 0).sum())
        fixed = max(1, used // 4)
        moved = fixed + (places - fixed + rotation * (used - fixed)) % max(1, count - fixed)
        return jnp.zeros((count,), jnp.int32).at[order[jnp.where(places < fixed, places, moved)]].set(jnp.asarray(lengths, jnp.int32))

    lengths = jnp.where(number % 4 == 0, named(crowded, number // 4), named(common, number - number // 4 - 1))
    mixed = jax.random.permutation(jax.random.fold_in(own, 3), count)
    donor, sink = mixed[0:count // 2 * 2:2], mixed[1:count // 2 * 2:2]
    slack = jnp.minimum(lengths[donor] - 1, reach - lengths[sink]) // 2
    slack = jnp.where((donor == order[0]) | (sink == order[0]) | (lengths[sink] == 0), 0, jnp.maximum(slack, 0))
    moved = jax.random.randint(jax.random.fold_in(own, 4), (count // 2,), 0, 1 << 20) % (slack + 1)
    lengths = lengths.at[donor].add(-moved).at[sink].add(moved)
    labels = jnp.searchsorted(jnp.cumsum(lengths), jnp.arange(rows * top), side="right").astype(jnp.int32)
    table = labels.reshape(top, rows).T
    table = table[jax.random.permutation(jax.random.fold_in(own, 1), rows)]
    rotation = jax.random.randint(jax.random.fold_in(own, 2), (rows, 1), 0, top)
    return jnp.take_along_axis(table, (jnp.arange(top)[None, :] + rotation) % top, axis=1)


def shares(count, total, most, lean, full):
    portions = [(1 << 20) // math.isqrt(rank ** lean) + 1 for rank in range(1, count + 1)]
    largest = most if full else min(most, max(-(-total // count), total * portions[0] // sum(portions)))
    least = 1 if total - largest >= count - 1 else 0
    counts, rest = [largest] + [least] * (count - 1), total - largest - least * (count - 1)
    while rest > 0:
        movable = [i for i in range(1, count) if counts[i] < largest] or [i for i in range(1, count) if counts[i] < most]
        mass, budget = sum([portions[i] for i in movable]), rest
        for i in movable:
            addition = min(most - counts[i], max(1, budget * portions[i] // mass), rest)
            counts[i] = counts[i] + addition
            rest = rest - addition
    return np.array(counts)


def scatter_about(key, shape, width, most, cuts=(), held_as=jnp.bfloat16):
    entries = width * jax.random.normal(key, shape, jnp.float32)
    if cuts:
        entries = entries * level_of(key, shape, cuts, -0.22, 0.18)
    return jnp.clip(entries, -most, most).astype(held_as)


def setup_inputs(seed: int = 0) -> dict:
    seeds = jax.random.split(jax.random.key(seed), 11)
    trained_gate = scatter_about(seeds[0], (EXPERTS, FF, D), D ** -0.5, 0.125, ((1, 2), (2, 16)), jnp.float32)
    trained_up = scatter_about(seeds[1], (EXPERTS, FF, D), D ** -0.5, 0.125, ((1, 2), (2, 16)), jnp.float32)
    trained_down = scatter_about(seeds[2], (EXPERTS, FF, D), FF ** -0.5, 0.25, ((1, 2), (2, 16)), jnp.float32)
    trained_shared_gate = scatter_about(seeds[3], (FF, D), D ** -0.5, 0.125, ((0, 2), (1, 16)), jnp.float32)
    trained_shared_up = scatter_about(seeds[4], (FF, D), D ** -0.5, 0.125, ((0, 2), (1, 16)), jnp.float32)
    trained_shared_down = scatter_about(seeds[5], (FF, D), FF ** -0.5, 0.25, ((0, 2), (1, 16)), jnp.float32)
    ffn_gain = jnp.clip(1.0 + 0.18 * jax.random.normal(seeds[6], (D,), jnp.float32), 0.1, 1.9)
    prompt_tokens = scatter_about(seeds[7], (TOKENS, D), 1.0, 6.0, ((0, 2),))
    expert_ids_keys = jax.random.split(jax.random.fold_in(seeds[8], 1), TOKENS // TOK)
    expert_ids_turns = jax.random.permutation(jax.random.fold_in(seeds[8], 3), TOKENS // TOK)
    expert_ids = jax.vmap(lambda own, number: assign_block(jax.random.fold_in(seeds[8], 2), own, number, TOK, EXPERTS, TOP_K, CAP, 1))(expert_ids_keys, expert_ids_turns).reshape((TOKENS, TOP_K))
    route_scores = jnp.clip(jnp.exp(math.log(1.0) - 2.9957323 * jax.random.uniform(seeds[9], (TOKENS, TOP_K), jnp.float32) ** level_of(seeds[9], (TOKENS, TOP_K), ((0, 2),), -0.2, 0.2)), 0.05, 1.0)
    return {"trained_gate": trained_gate, "trained_up": trained_up, "trained_down": trained_down, "trained_shared_gate": trained_shared_gate, "trained_shared_up": trained_shared_up, "trained_shared_down": trained_shared_down, "ffn_gain": ffn_gain, "prompt_tokens": prompt_tokens, "expert_ids": expert_ids, "route_scores": route_scores}


EPSILON = 1e-06
ROUTED_SCALE = 2.5

def contract(left, right):
    return lax.dot_general(left, right, (((1,), (1,)), ((), ())), preferred_element_type=jnp.float32)

def reference(trained_gate, trained_up, trained_down, trained_shared_gate, trained_shared_up, trained_shared_down, ffn_gain, prompt_tokens, expert_ids, route_scores):
    served_gate = (trained_gate * ffn_gain[None, None, :]).astype(jnp.bfloat16)
    served_up = (trained_up * ffn_gain[None, None, :]).astype(jnp.bfloat16)
    served_down = trained_down.astype(jnp.bfloat16)
    served_shared_gate = (trained_shared_gate * ffn_gain[None, :]).astype(jnp.bfloat16)
    served_shared_up = (trained_shared_up * ffn_gain[None, :]).astype(jnp.bfloat16)
    served_shared_down = trained_shared_down.astype(jnp.bfloat16)
    tokens_float = prompt_tokens.astype(jnp.float32)
    normed = (tokens_float * lax.rsqrt(lax.optimization_barrier(jnp.mean(tokens_float * tokens_float, axis=1, keepdims=True)) + EPSILON)).astype(jnp.bfloat16)
    route_weight = ROUTED_SCALE * route_scores / lax.optimization_barrier(jnp.sum(route_scores, axis=1, keepdims=True))
    token_total = prompt_tokens.shape[0]
    slot_total = N_FS * CAP
    token_range = jnp.arange(token_total, dtype=jnp.int32)

    def one_expert(routed, inputs):
        expert_index, gate_weight, up_weight, down_weight = inputs
        chosen = expert_ids == expert_index
        token_weight = lax.optimization_barrier(jnp.sum(jnp.where(chosen, route_weight, 0.0), axis=1))
        present = jnp.any(chosen, axis=1)
        position = (jnp.cumsum(present.astype(jnp.int32)) - 1).astype(jnp.int32)
        target = jnp.where(present, position, slot_total).astype(jnp.int32)
        slot_token = jnp.zeros((slot_total + 1,), jnp.int32).at[target].set(token_range)[:slot_total]
        slot_rows = jnp.take(normed, slot_token, axis=0)
        gate_pre = contract(slot_rows, gate_weight)
        up_pre = contract(slot_rows, up_weight)
        expert_act = (jax.nn.silu(gate_pre) * up_pre).astype(jnp.bfloat16)
        expert_out = jnp.dot(expert_act, down_weight, preferred_element_type=jnp.float32)
        picked = jnp.take(expert_out, jnp.maximum(position, 0), axis=0)
        return (routed + jnp.where(present[:, None], picked * token_weight[:, None], 0.0), None)
    expert_range = jnp.arange(EXPERTS, dtype=jnp.int32)
    routed, _ = lax.scan(one_expert, jnp.zeros((token_total, D), jnp.float32), (expert_range, served_gate, served_up, served_down))
    shared_gate_pre = contract(normed, served_shared_gate)
    shared_up_pre = contract(normed, served_shared_up)
    shared_act = (jax.nn.silu(shared_gate_pre) * shared_up_pre).astype(jnp.bfloat16)
    shared_out = jnp.dot(shared_act, served_shared_down, preferred_element_type=jnp.float32)
    mixture_out = (routed + shared_out).astype(jnp.bfloat16)
    return (served_gate, served_up, served_down, served_shared_gate, served_shared_up, served_shared_down, mixture_out)
```

```python
import functools

import jax
import jax.numpy as jnp
from jax import lax
from jax.experimental import pallas as pl
from jax.experimental.pallas import tpu as pltpu
from jax.sharding import PartitionSpec as P

EPSILON = 1e-06
ROUTED_SCALE = 2.5
SUBLANES = 16


def round_up(value, multiple):
    return -(-value // multiple) * multiple


def activation_kernel(normed_ref, gate_ref, up_ref, weight_ref, out_ref, *, shared_rows):
    blocks, _, width = gate_ref.shape
    step = 2 if blocks % 2 == 0 else 1

    def product(ref):
        total = None
        for start in range(0, blocks, step):
            left = normed_ref[:, start * width : (start + step) * width]
            right = jnp.concatenate([ref[start + i] for i in range(step)], axis=1)
            part = lax.dot_general(
                left, right, (((1,), (1,)), ((), ())), preferred_element_type=jnp.float32
            )
            total = part if total is None else total + part
        return total

    gate = product(gate_ref)
    up = product(up_ref)
    act = gate / (1.0 + jnp.exp(-gate)) * up
    unit = lax.broadcasted_iota(jnp.int32, act.shape, 1)
    act = act * jnp.where(unit < shared_rows, 1.0, weight_ref[...])
    out_ref[...] = act.astype(out_ref.dtype)


def activation(normed, gate, up, weight, shared_rows):
    return pl.pallas_call(
        functools.partial(activation_kernel, shared_rows=shared_rows),
        out_shape=jax.ShapeDtypeStruct((normed.shape[0], gate.shape[1]), jnp.bfloat16),
    )(normed, gate, up, weight)


def down_kernel(*refs):
    count = len(refs) // 2
    total = None
    for act_ref, down_ref in zip(refs[:count], refs[count : 2 * count]):
        part = jnp.dot(act_ref[...], down_ref[0], preferred_element_type=jnp.float32)
        total = part if total is None else total + part
    refs[-1][0] = total.astype(refs[-1].dtype)


def down_product(acts, downs):
    blocks, rows, width = downs[0].shape
    tokens = acts[0].shape[0]
    return pl.pallas_call(
        down_kernel,
        grid=(blocks,),
        in_specs=[pl.BlockSpec((tokens, rows), lambda s: (0, 0)) for _ in acts]
        + [pl.BlockSpec((1, rows, width), lambda s: (s, 0, 0)) for _ in downs],
        out_specs=pl.BlockSpec((1, tokens, width), lambda s: (s, 0, 0)),
        out_shape=jax.ShapeDtypeStruct((blocks, tokens, width), jnp.bfloat16),
    )(*acts, *downs)


def pick(array, index, axis):
    return lax.dynamic_index_in_dim(array, index, axis, keepdims=False)


def halve(array, index, bit, axis, size):
    partner = [(s, s ^ bit) for s in range(size)]
    mine = (index // bit) % 2
    arrived = lax.ppermute(pick(array, 1 - mine, axis), "tp", partner)
    total = pick(array, mine, axis).astype(jnp.float32) + arrived.astype(jnp.float32)
    return total.astype(array.dtype)


def reduce_blocks(partial):
    size, tokens, width = partial.shape
    index = lax.axis_index("tp")
    if size % 4:
        arrived = lax.all_to_all(partial, "tp", 0, 0, tiled=True)
        return jnp.sum(arrived.astype(jnp.float32), axis=0)
    outer = size // 4
    grid = partial.reshape(outer, 2, 2, tokens, width)
    half = tokens // 2
    first, second = grid[:, :, :, :half], grid[:, :, :, half:]
    first = halve(first, index, 1, 2, size)
    second = halve(second, index, 2, 1, size)
    first = halve(first, index, 2, 1, size)
    second = halve(second, index, 1, 1, size)
    both = jnp.concatenate([first, second], axis=1)
    plane = index // 4
    total = pick(both, plane, 0).astype(jnp.float32)
    for shift in range(1, outer):
        send = pick(both, (plane + shift) % outer, 0)
        arrived = lax.ppermute(send, "tp", [(s, (s + 4 * shift) % size) for s in range(size)])
        total = total + arrived.astype(jnp.float32)
    return total


def on_device(
    trained_gate,
    trained_up,
    trained_down,
    trained_shared_gate,
    trained_shared_up,
    trained_shared_down,
    ffn_gain,
    prompt_tokens,
    expert_ids,
    route_scores,
):
    tp_size, fs_size = lax.axis_size("tp"), lax.axis_size("fs")
    tp_index, fs_index = lax.axis_index("tp"), lax.axis_index("fs")
    hidden = trained_gate.shape[1]
    dealt = -(-hidden // tp_size)
    shared_rows = round_up(dealt, SUBLANES)
    rows = round_up(shared_rows + hidden, SUBLANES)
    bf16 = jnp.bfloat16

    def deal(shared):
        padded = jnp.pad(shared, ((0, dealt * tp_size - hidden), (0, 0)))
        return padded.reshape(tp_size, dealt, shared.shape[1])

    def pack(routed, shared):
        top = jnp.pad(deal(shared), ((0, 0), (0, shared_rows - dealt), (0, 0)))
        bottom = jnp.pad(routed, ((0, 0), (0, rows - shared_rows - hidden), (0, 0)))
        return jnp.concatenate([top, bottom], axis=1)

    sgate = (trained_shared_gate * ffn_gain[None, :]).astype(bf16)
    sup = (trained_shared_up * ffn_gain[None, :]).astype(bf16)
    sdown = trained_shared_down.astype(bf16)
    packed = (
        pack((trained_gate * ffn_gain[None, None, :]).astype(bf16), sgate),
        pack((trained_up * ffn_gain[None, None, :]).astype(bf16), sup),
        pack(trained_down.astype(bf16), sdown),
    )

    def exchange(array):
        if fs_size == 2:
            other = lax.ppermute(array, "fs", [(0, 1), (1, 0)])
            low = jnp.where(fs_index == 0, array, other)
            high = jnp.where(fs_index == 0, other, array)
            return (array, other), (low, high)
        whole = lax.all_gather(array, "fs", axis=0, tiled=False)
        parts = tuple(whole[i] for i in range(fs_size))
        return parts, parts

    def spread(array):
        return lax.all_to_all(array, "tp", split_axis=0, concat_axis=0, tiled=True)

    def served(ordered):
        kept = [part[:, shared_rows : shared_rows + hidden] for part in ordered]
        whole = jnp.concatenate(kept, axis=1)
        return whole.transpose(1, 0, 2).reshape(1, whole.shape[1], -1)

    gates, gates_ordered = exchange(spread(packed[0]))
    ups, ups_ordered = exchange(spread(packed[1]))
    downs, downs_ordered = exchange(spread(packed[2]))

    tokens_float = prompt_tokens.astype(jnp.float32)
    normed = (
        tokens_float
        * lax.rsqrt(jnp.mean(tokens_float * tokens_float, axis=1, keepdims=True) + EPSILON)
    ).astype(bf16)
    chosen = jnp.where(expert_ids == tp_index, route_scores, 0.0)
    weight = (
        ROUTED_SCALE
        * jnp.sum(chosen, axis=1, keepdims=True)
        / jnp.sum(route_scores, axis=1, keepdims=True)
    )
    acts = [activation(normed, g, u, weight, shared_rows) for g, u in zip(gates, ups)]
    mixture = reduce_blocks(down_product(acts, downs)).astype(bf16)

    shared_served = []
    for array in (sgate, sup, sdown):
        _, ordered = exchange(array)
        shared_served.append(jnp.concatenate(ordered, axis=0))
    return (
        served(gates_ordered),
        served(ups_ordered),
        served(downs_ordered),
        *shared_served,
        mixture,
    )


def solution(mesh):
    placed = (
        P(None, "fs", "tp"),
        P(None, "fs", "tp"),
        P(None, "fs", "tp"),
        P("fs", "tp"),
        P("fs", "tp"),
        P("fs", "tp"),
        P("tp"),
        P("fs", None),
        P("fs", None),
        P("fs", None),
    )
    return jax.shard_map(
        on_device,
        mesh=mesh,
        in_specs=placed,
        out_specs=(
            P("tp", None, None),
            P("tp", None, None),
            P("tp", None, None),
            P(None, "tp"),
            P(None, "tp"),
            P(None, "tp"),
            P("fs", "tp"),
        ),
        check_vma=False,
    )
```

```python
import functools

import jax
import jax.numpy as jnp
from jax import lax
from jax.experimental import pallas as pl
from jax.experimental.pallas import tpu as pltpu
from jax.sharding import PartitionSpec as P

EPSILON = 1e-06
ROUTED_SCALE = 2.5
SUBLANES = 16


def round_up(value, multiple):
    return -(-value // multiple) * multiple


def activation_kernel(normed_ref, pair_ref, weight_ref, out_ref, *, shared_rows):
    blocks, both, width = pair_ref.shape
    rows = both // 2
    step = 2 if blocks % 2 == 0 else 1

    def product(offset):
        total = None
        for start in range(0, blocks, step):
            left = normed_ref[:, start * width : (start + step) * width]
            right = jnp.concatenate(
                [pair_ref[start + i, offset : offset + rows] for i in range(step)], axis=1
            )
            part = lax.dot_general(
                left, right, (((1,), (1,)), ((), ())), preferred_element_type=jnp.float32
            )
            total = part if total is None else total + part
        return total

    gate = product(0)
    up = product(rows)
    act = gate / (1.0 + jnp.exp(-gate)) * up
    unit = lax.broadcasted_iota(jnp.int32, act.shape, 1)
    act = act * jnp.where(unit < shared_rows, 1.0, weight_ref[...])
    out_ref[...] = act.astype(out_ref.dtype)


def activation(normed, pair, weight, shared_rows):
    return pl.pallas_call(
        functools.partial(activation_kernel, shared_rows=shared_rows),
        out_shape=jax.ShapeDtypeStruct((normed.shape[0], pair.shape[1] // 2), jnp.bfloat16),
    )(normed, pair, weight)


def down_kernel(bits_ref, *refs, count):
    act_refs, down_refs = refs[:count], refs[count : 2 * count]
    keep_first, send_first, keep_second, send_second = refs[2 * count :]
    outer, _, half, width = keep_first.shape
    mine_x, mine_y = bits_ref[0] == 0, bits_ref[1] == 0
    acts = [ref[...] for ref in act_refs]
    for plane in range(outer):
        products = []
        for y in range(2):
            total = None
            for act, ref in zip(acts, down_refs):
                base = plane * 4 + y * 2
                right = jnp.concatenate([ref[base], ref[base + 1]], axis=1)
                part = jnp.dot(act, right, preferred_element_type=jnp.float32)
                total = part if total is None else total + part
            low, high = total[:half, :width], total[:half, width:]
            keep_first[plane, y] = jnp.where(mine_x, low, high)
            send_first[plane, y] = jnp.where(mine_x, high, low).astype(send_first.dtype)
            products.append(total[half:])
        keep = jnp.where(mine_y, products[0], products[1])
        send = jnp.where(mine_y, products[1], products[0]).astype(send_second.dtype)
        for x in range(2):
            keep_second[plane, x] = keep[:, x * width : (x + 1) * width]
            send_second[plane, x] = send[:, x * width : (x + 1) * width]


def down_product(acts, downs, bits):
    blocks, _, width = downs[0].shape
    shape = (blocks // 4, 2, acts[0].shape[0] // 2, width)
    keep = jax.ShapeDtypeStruct(shape, jnp.float32)
    send = jax.ShapeDtypeStruct(shape, jnp.bfloat16)
    vmem = [pl.BlockSpec(memory_space=pltpu.VMEM) for _ in (*acts, *downs)]
    return pl.pallas_call(
        functools.partial(down_kernel, count=len(acts)),
        in_specs=[pl.BlockSpec(memory_space=pltpu.SMEM), *vmem],
        out_shape=(keep, send, keep, send),
    )(bits, *acts, *downs)


def serve_kernel(swap_ref, *refs, count, offsets, hidden):
    scratch = refs[-1]
    parts, outs = refs[:count], refs[count:-1]
    chunk, _, width = parts[0].shape
    swapped = swap_ref[0] == 1
    for offset, out in zip(offsets, outs):
        for i in range(chunk):
            pieces = [part[i, offset : offset + hidden].astype(jnp.float32) for part in parts]
            if count == 2:
                pieces = [
                    jnp.where(swapped, pieces[1], pieces[0]),
                    jnp.where(swapped, pieces[0], pieces[1]),
                ]
            for place, piece in enumerate(pieces):
                scratch[place * hidden : (place + 1) * hidden] = piece
            out[0, :, i * width : (i + 1) * width] = scratch[...].astype(out.dtype)


def serve(parts, swap, offsets, hidden):
    blocks, rows, width = parts[0].shape
    chunk = 4 if blocks % 4 == 0 else 1
    total = hidden * len(parts)
    return pl.pallas_call(
        functools.partial(serve_kernel, count=len(parts), offsets=offsets, hidden=hidden),
        grid=(blocks // chunk,),
        in_specs=[pl.BlockSpec(memory_space=pltpu.SMEM)]
        + [pl.BlockSpec((chunk, rows, width), lambda s: (s, 0, 0)) for _ in parts],
        out_specs=[pl.BlockSpec((1, total, chunk * width), lambda s: (0, 0, s)) for _ in offsets],
        out_shape=[
            jax.ShapeDtypeStruct((1, total, blocks * width), jnp.bfloat16) for _ in offsets
        ],
        scratch_shapes=[pltpu.VMEM((total, width), jnp.float32)],
    )(swap, *parts)


def pick(array, index, axis):
    return lax.dynamic_index_in_dim(array, index, axis, keepdims=False)


def flip(array, bit, size):
    return lax.ppermute(array, "tp", [(s, s ^ bit) for s in range(size)])


def reduce_blocks(parts, size, index):
    keep_first, send_first, keep_second, send_second = parts
    outer = size // 4
    x, y, plane = index % 2, (index // 2) % 2, index // 4
    first = keep_first + flip(send_first, 1, size)
    second = keep_second + flip(send_second, 2, size)
    half = jnp.bfloat16
    first = pick(first, y, 1) + flip(pick(first, 1 - y, 1).astype(half), 2, size)
    second = pick(second, x, 1) + flip(pick(second, 1 - x, 1).astype(half), 1, size)
    both = jnp.concatenate([first, second], axis=1)
    rounded = both.astype(half)
    total = pick(both, plane, 0)
    for shift in range(1, outer):
        send = pick(rounded, (plane + shift) % outer, 0)
        total = total + lax.ppermute(
            send, "tp", [(s, (s + 4 * shift) % size) for s in range(size)]
        )
    return total


def on_device(
    trained_gate,
    trained_up,
    trained_down,
    trained_shared_gate,
    trained_shared_up,
    trained_shared_down,
    ffn_gain,
    prompt_tokens,
    expert_ids,
    route_scores,
):
    tp_size, fs_size = lax.axis_size("tp"), lax.axis_size("fs")
    tp_index, fs_index = lax.axis_index("tp"), lax.axis_index("fs")
    hidden = trained_gate.shape[1]
    dealt = -(-hidden // tp_size)
    shared_rows = round_up(dealt, SUBLANES)
    rows = round_up(shared_rows + hidden, SUBLANES)
    bf16 = jnp.bfloat16

    def deal(shared):
        padded = jnp.pad(shared, ((0, dealt * tp_size - hidden), (0, 0)))
        return padded.reshape(tp_size, dealt, shared.shape[1])

    def pack(routed, shared):
        top = jnp.pad(deal(shared), ((0, 0), (0, shared_rows - dealt), (0, 0)))
        bottom = jnp.pad(routed, ((0, 0), (0, rows - shared_rows - hidden), (0, 0)))
        return jnp.concatenate([top, bottom], axis=1)

    sgate = (trained_shared_gate * ffn_gain[None, :]).astype(bf16)
    sup = (trained_shared_up * ffn_gain[None, :]).astype(bf16)
    sdown = trained_shared_down.astype(bf16)
    pair = jnp.concatenate(
        [
            pack((trained_gate * ffn_gain[None, None, :]).astype(bf16), sgate),
            pack((trained_up * ffn_gain[None, None, :]).astype(bf16), sup),
        ],
        axis=1,
    )

    def exchange(array):
        if fs_size == 2:
            return array, lax.ppermute(array, "fs", [(0, 1), (1, 0)])
        whole = lax.all_gather(array, "fs", axis=0, tiled=False)
        return tuple(whole[i] for i in range(fs_size))

    def spread(array):
        return lax.all_to_all(array, "tp", split_axis=0, concat_axis=0, tiled=True)

    swap = jnp.reshape(fs_index, (1,)).astype(jnp.int32)
    bits = jnp.stack([tp_index % 2, (tp_index // 2) % 2]).astype(jnp.int32)
    tokens_float = prompt_tokens.astype(jnp.float32)
    normed = (
        tokens_float
        * lax.rsqrt(jnp.mean(tokens_float * tokens_float, axis=1, keepdims=True) + EPSILON)
    ).astype(bf16)
    chosen = jnp.where(expert_ids == tp_index, route_scores, 0.0)
    weight = (
        ROUTED_SCALE
        * jnp.sum(chosen, axis=1, keepdims=True)
        / jnp.sum(route_scores, axis=1, keepdims=True)
    )

    pairs = exchange(spread(pair))
    acts = tuple(activation(normed, p, weight, shared_rows) for p in pairs)
    served_gate, served_up = serve(pairs, swap, (shared_rows, rows + shared_rows), hidden)
    down = spread(pack(trained_down.astype(bf16), sdown))

    shared_served = []
    for array in (sgate, sup, sdown):
        parts = exchange(array)
        if fs_size == 2:
            own, other = parts
            parts = (
                jnp.where(fs_index == 0, own, other),
                jnp.where(fs_index == 0, other, own),
            )
        shared_served.append(jnp.concatenate(parts, axis=0))

    down, acts, served_gate, served_up, shared_served = lax.optimization_barrier(
        (down, acts, served_gate, served_up, shared_served)
    )
    downs = exchange(down)
    mixture = reduce_blocks(down_product(acts, downs, bits), tp_size, tp_index).astype(bf16)
    (served_down,) = serve(downs, swap, (shared_rows,), hidden)
    return (served_gate, served_up, served_down, *shared_served, mixture)


def solution(mesh):
    placed = (
        P(None, "fs", "tp"),
        P(None, "fs", "tp"),
        P(None, "fs", "tp"),
        P("fs", "tp"),
        P("fs", "tp"),
        P("fs", "tp"),
        P("tp"),
        P("fs", None),
        P("fs", None),
        P("fs", None),
    )
    return jax.shard_map(
        on_device,
        mesh=mesh,
        in_specs=placed,
        out_specs=(
            P("tp", None, None),
            P("tp", None, None),
            P("tp", None, None),
            P(None, "tp"),
            P(None, "tp"),
            P(None, "tp"),
            P("fs", "tp"),
        ),
        check_vma=False,
    )
```

```python
import functools

import jax
import jax.numpy as jnp
from jax import lax
from jax.experimental import pallas as pl
from jax.experimental.pallas import tpu as pltpu
from jax.sharding import PartitionSpec as P

EPSILON = 1e-06
ROUTED_SCALE = 2.5
SUBLANES = 16


def round_up(value, multiple):
    return -(-value // multiple) * multiple


def activation_kernel(normed_ref, pair_ref, weight_ref, out_ref, *, shared_rows):
    blocks, both, width = pair_ref.shape
    rows = both // 2
    step = 2 if blocks % 2 == 0 else 1

    def product(offset):
        total = None
        for start in range(0, blocks, step):
            left = normed_ref[:, start * width : (start + step) * width]
            right = jnp.concatenate(
                [pair_ref[start + i, offset : offset + rows] for i in range(step)], axis=1
            )
            part = lax.dot_general(
                left, right, (((1,), (1,)), ((), ())), preferred_element_type=jnp.float32
            )
            total = part if total is None else total + part
        return total

    gate = product(0)
    up = product(rows)
    act = gate / (1.0 + jnp.exp(-gate)) * up
    unit = lax.broadcasted_iota(jnp.int32, act.shape, 1)
    act = act * jnp.where(unit < shared_rows, 1.0, weight_ref[...])
    out_ref[...] = act.astype(out_ref.dtype)


def activation(normed, pair, weight, shared_rows):
    return pl.pallas_call(
        functools.partial(activation_kernel, shared_rows=shared_rows),
        out_shape=jax.ShapeDtypeStruct((normed.shape[0], pair.shape[1] // 2), jnp.bfloat16),
    )(normed, pair, weight)


def down_kernel(bits_ref, act_ref, *refs):
    down_refs = refs[:-4]
    keep_first, send_first, keep_second, send_second = refs[-4:]
    _, outer, half, width = keep_first.shape
    mine_x, mine_y = bits_ref[0] == 0, bits_ref[1] == 0
    act = act_ref[...]
    for plane in range(outer):
        products = []
        for y in range(2):
            base = plane * 4 + y * 2
            right = jnp.concatenate(
                [
                    jnp.concatenate([ref[base + x] for ref in down_refs], axis=0)
                    for x in range(2)
                ],
                axis=1,
            )
            total = jnp.dot(act, right, preferred_element_type=jnp.float32)
            low, high = total[:half, :width], total[:half, width:]
            keep_first[y, plane] = jnp.where(mine_x, low, high)
            send_first[y, plane] = jnp.where(mine_x, high, low).astype(send_first.dtype)
            products.append(total[half:])
        keep = jnp.where(mine_y, products[0], products[1])
        send = jnp.where(mine_y, products[1], products[0]).astype(send_second.dtype)
        for x in range(2):
            keep_second[x, plane] = keep[:, x * width : (x + 1) * width]
            send_second[x, plane] = send[:, x * width : (x + 1) * width]


def down_product(acts, downs, bits):
    blocks, _, width = downs[0].shape
    shape = (2, blocks // 4, acts.shape[0] // 2, width)
    keep = jax.ShapeDtypeStruct(shape, jnp.float32)
    send = jax.ShapeDtypeStruct(shape, jnp.bfloat16)
    vmem = [pl.BlockSpec(memory_space=pltpu.VMEM) for _ in (acts, *downs)]
    return pl.pallas_call(
        down_kernel,
        in_specs=[pl.BlockSpec(memory_space=pltpu.SMEM), *vmem],
        out_shape=(keep, send, keep, send),
    )(bits, acts, *downs)


def serve_kernel(swap_ref, *refs, count, offsets, hidden):
    scratch = refs[-1]
    parts, outs = refs[:count], refs[count:-1]
    chunk, _, width = parts[0].shape
    swapped = swap_ref[0] == 1
    for offset, out in zip(offsets, outs):
        for i in range(chunk):
            pieces = [part[i, offset : offset + hidden].astype(jnp.float32) for part in parts]
            if count == 2:
                pieces = [
                    jnp.where(swapped, pieces[1], pieces[0]),
                    jnp.where(swapped, pieces[0], pieces[1]),
                ]
            for place, piece in enumerate(pieces):
                scratch[place * hidden : (place + 1) * hidden] = piece
            out[0, :, i * width : (i + 1) * width] = scratch[...].astype(out.dtype)


def serve(parts, swap, offsets, hidden):
    blocks, rows, width = parts[0].shape
    chunk = 4 if blocks % 4 == 0 else 1
    total = hidden * len(parts)
    return pl.pallas_call(
        functools.partial(serve_kernel, count=len(parts), offsets=offsets, hidden=hidden),
        grid=(blocks // chunk,),
        in_specs=[pl.BlockSpec(memory_space=pltpu.SMEM)]
        + [pl.BlockSpec((chunk, rows, width), lambda s: (s, 0, 0)) for _ in parts],
        out_specs=[pl.BlockSpec((1, total, chunk * width), lambda s: (0, 0, s)) for _ in offsets],
        out_shape=[
            jax.ShapeDtypeStruct((1, total, blocks * width), jnp.bfloat16) for _ in offsets
        ],
        scratch_shapes=[pltpu.VMEM((total, width), jnp.float32)],
    )(swap, *parts)


def pick(array, index, axis):
    return lax.dynamic_index_in_dim(array, index, axis, keepdims=False)


def flip(array, bit, size):
    return lax.ppermute(array, "tp", [(s, s ^ bit) for s in range(size)])


def reduce_blocks(parts, size, index):
    keep_first, send_first, keep_second, send_second = parts
    outer = size // 4
    x, y, plane = index % 2, (index // 2) % 2, index // 4
    first = keep_first + flip(send_first, 1, size)
    second = keep_second + flip(send_second, 2, size)
    half = jnp.bfloat16
    first = pick(first, y, 0) + flip(pick(first, 1 - y, 0).astype(half), 2, size)
    second = pick(second, x, 0) + flip(pick(second, 1 - x, 0).astype(half), 1, size)
    both = jnp.concatenate([first, second], axis=1)
    rounded = both.astype(half)
    total = pick(both, plane, 0)
    for shift in range(1, outer):
        send = pick(rounded, (plane + shift) % outer, 0)
        total = total + lax.ppermute(
            send, "tp", [(s, (s + 4 * shift) % size) for s in range(size)]
        )
    return total


def on_device(
    trained_gate,
    trained_up,
    trained_down,
    trained_shared_gate,
    trained_shared_up,
    trained_shared_down,
    ffn_gain,
    prompt_tokens,
    expert_ids,
    route_scores,
):
    tp_size, fs_size = lax.axis_size("tp"), lax.axis_size("fs")
    tp_index, fs_index = lax.axis_index("tp"), lax.axis_index("fs")
    hidden = trained_gate.shape[1]
    dealt = -(-hidden // tp_size)
    shared_rows = round_up(dealt, SUBLANES)
    rows = round_up(shared_rows + hidden, SUBLANES)
    bf16 = jnp.bfloat16

    def deal(shared):
        padded = jnp.pad(shared, ((0, dealt * tp_size - hidden), (0, 0)))
        return padded.reshape(tp_size, dealt, shared.shape[1])

    def top(shared):
        return jnp.pad(deal(shared), ((0, 0), (0, shared_rows - dealt), (0, 0)))

    def pack(routed, shared):
        bottom = jnp.pad(routed, ((0, 0), (0, rows - shared_rows - hidden), (0, 0)))
        return jnp.concatenate([top(shared), bottom], axis=1)

    sgate = (trained_shared_gate * ffn_gain[None, :]).astype(bf16)
    sup = (trained_shared_up * ffn_gain[None, :]).astype(bf16)
    sdown = trained_shared_down.astype(bf16)
    pair = jnp.concatenate(
        [
            pack((trained_gate * ffn_gain[None, None, :]).astype(bf16), sgate),
            pack((trained_up * ffn_gain[None, None, :]).astype(bf16), sup),
        ],
        axis=1,
    )

    def exchange(array):
        if fs_size == 2:
            return array, lax.ppermute(array, "fs", [(0, 1), (1, 0)])
        whole = lax.all_gather(array, "fs", axis=0, tiled=False)
        return tuple(whole[i] for i in range(fs_size))

    def spread(array):
        return lax.all_to_all(array, "tp", split_axis=0, concat_axis=0, tiled=True)

    swap = jnp.reshape(fs_index, (1,)).astype(jnp.int32)
    bits = jnp.stack([tp_index % 2, (tp_index // 2) % 2]).astype(jnp.int32)
    tokens_float = prompt_tokens.astype(jnp.float32)
    normed = (
        tokens_float
        * lax.rsqrt(jnp.mean(tokens_float * tokens_float, axis=1, keepdims=True) + EPSILON)
    ).astype(bf16)
    chosen = jnp.where(expert_ids == tp_index, route_scores, 0.0)
    weight = (
        ROUTED_SCALE
        * jnp.sum(chosen, axis=1, keepdims=True)
        / jnp.sum(route_scores, axis=1, keepdims=True)
    )

    arrived, down_packed, normed, weight = lax.optimization_barrier(
        (spread(pair), pack(trained_down.astype(bf16), sdown), normed, weight)
    )
    pairs = exchange(arrived)
    acts = jnp.concatenate([activation(normed, p, weight, shared_rows) for p in pairs], axis=1)
    served_gate, served_up = serve(pairs, swap, (shared_rows, rows + shared_rows), hidden)
    down = spread(down_packed)

    shared_served = []
    for array in (sgate, sup, sdown):
        parts = exchange(array)
        if fs_size == 2:
            own, other = parts
            parts = (
                jnp.where(fs_index == 0, own, other),
                jnp.where(fs_index == 0, other, own),
            )
        shared_served.append(jnp.concatenate(parts, axis=0))

    down, acts, served_gate, served_up, shared_served, bits = lax.optimization_barrier(
        (down, acts, served_gate, served_up, shared_served, bits)
    )
    downs = exchange(down)
    mixture = reduce_blocks(down_product(acts, downs, bits), tp_size, tp_index).astype(bf16)
    (served_down,) = serve(downs, swap, (shared_rows,), hidden)
    return (served_gate, served_up, served_down, *shared_served, mixture)


def solution(mesh):
    placed = (
        P(None, "fs", "tp"),
        P(None, "fs", "tp"),
        P(None, "fs", "tp"),
        P("fs", "tp"),
        P("fs", "tp"),
        P("fs", "tp"),
        P("tp"),
        P("fs", None),
        P("fs", None),
        P("fs", None),
    )
    return jax.shard_map(
        on_device,
        mesh=mesh,
        in_specs=placed,
        out_specs=(
            P("tp", None, None),
            P("tp", None, None),
            P("tp", None, None),
            P(None, "tp"),
            P(None, "tp"),
            P(None, "tp"),
            P("fs", "tp"),
        ),
        check_vma=False,
    )
```
